128 devices in a mesh: ep: 128 (over z, y, x, core).
Axes of the slice: x: 4, y: 4, z: 4, core: 2. Of those that a mesh axis runs over, the one named last changes fastest.
Arguments:
- hidden_in: bfloat16 [256, 2048], P('ep'), may hold values from -6 to 6
- lengths: int32 [256], P('ep'), may hold values from 1 to 1024, as said below
- key_cache: bfloat16 [256, 1024, 512], P('ep'), may hold values from -30 to 30
- value_cache: bfloat16 [256, 1024, 512], P('ep'), may hold values from -6 to 6
- query_w: bfloat16 [2048, 2048], P('ep'), may hold values from -0.125 to 0.125
- key_w: bfloat16 [2048, 512], P('ep'), may hold values from -0.125 to 0.125
- value_w: bfloat16 [2048, 512], P('ep'), may hold values from -0.125 to 0.125
- out_w: bfloat16 [2048, 2048], P('ep'), may hold values from -0.125 to 0.125
- lam_heads: float32 [8], replicated, may hold values from 0.3 to 0.8
- head_gain: float32 [256], replicated, may hold values from 0.1 to 1.9
- attn_gain: float32 [2048], replicated, may hold values from 0.1 to 1.9
- moe_gain: float32 [2048], replicated, may hold values from 0.1 to 1.9
- routing: int32 [256, 6], replicated, may hold values from 0 to 127, all different within a row; in each aligned block of 256 rows (0 to 255, 256 to 511, ...) at most 24 rows name the same one
- route_weight: float32 [256, 6], replicated, may hold values from 0.1 to 0.6
- gate_w: bfloat16 [128, 2048, 512], P('ep'), may hold values from -0.125 to 0.125
- up_w: bfloat16 [128, 2048, 512], P('ep'), may hold values from -0.125 to 0.125
- down_w: bfloat16 [128, 512, 2048], P('ep'), may hold values from -0.25 to 0.25
- shared_gate: bfloat16 [2048, 512], replicated, may hold values from -0.125 to 0.125
- shared_up: bfloat16 [2048, 512], replicated, may hold values from -0.125 to 0.125
- shared_down: bfloat16 [512, 2048], replicated, may hold values from -0.25 to 0.25
Outputs:
- layer_out: bfloat16 [256, 2048], P('ep')
- key_new: bfloat16 [256, 512], P('ep')
- value_new: bfloat16 [256, 512], P('ep')
The draws below stay inside these ranges and needn't reach their ends.
Inputs may be any that keep to these rules, and one draw needn't show every extreme that they name: `lengths`: some sequence has exactly 1024 positions in use. `routing`: each row names 6 different experts; no expert is named by more than 24 rows, a bound that some block reaches.
All inputs are finite; a program needn't handle non-finite values.
Results may differ from the reference program's by a relative error of at most 0.013.
The reference program's roundings to bfloat16 on the way count: a program that leaves them out, or rounds other values in their place, can miss the bound.
Values may be sent and summed in bfloat16 or wider, within the bound.
No kernel may reach another device: no remote copies, remote signals or barrier semaphores. Data moves between devices by JAX's collectives and lax.ppermute only.
A program may use at most 64 MiB of HBM per device.

```python
import math
import jax
import jax.numpy as jnp
import numpy as np
from jax import lax

D = 2048
HEADS = 8
KV_HEADS = 2
HEAD_DIM = 128
VALUE_DIM = 256
EXPERT_DIM = 512
SHARED_DIM = 512
TOPK = 6
CACHE = 1024
SEQS = 256
EXPERTS = 128
EXP_CAP = 24


def draw_lengths(key, part):
    first_key, second_key = jax.random.split(key, 2)
    drawn = jax.random.randint(first_key, (SEQS,), 1, CACHE + 1, jnp.int32)
    chosen = jax.random.randint(second_key, (), 0, SEQS, jnp.int32)
    return jnp.where(jnp.arange(SEQS, dtype=jnp.int32) == chosen, CACHE, drawn).astype(jnp.int32)


def draw_key_cache(key, part):
    first_key = jax.random.fold_in(key, 0)
    shape = (SEQS, CACHE, KV_HEADS * 2 * HEAD_DIM)
    drawn = jnp.clip(1.75 * jax.random.normal(first_key, shape, jnp.float32), -14.0, 14.0)
    return drawn.astype(jnp.bfloat16)


def block_levels(own_key, extent, cuts, smallest, high):
    factor_of = 1.0
    for axis_at, shards_of in cuts:
        heights = jax.random.uniform(jax.random.fold_in(jax.random.fold_in(own_key, 6), axis_at), (shards_of,), jnp.float32, smallest / len(cuts), high / len(cuts))
        factor_of = factor_of * jnp.repeat(jnp.exp(heights), extent[axis_at] // shards_of).reshape((-1,) + (1,) * (len(extent) - 1 - axis_at))
    return factor_of


def deal_out(stream_key, own, number, rows, count, top, reach, slope):
    ranking = jax.random.permutation(stream_key, count)
    packed, ordinary = shares(count, rows * top, reach, slope, True), shares(count, rows * top, reach, slope, False)
    places = jnp.arange(count)

    def named(tallies, offset_by):
        used = int((tallies > 0).sum())
        fixed = max(1, used // 4)
        shifted = fixed + (places - fixed + offset_by * (used - fixed)) % max(1, count - fixed)
        return jnp.zeros((count,), jnp.int32).at[ranking[jnp.where(places < fixed, places, shifted)]].set(jnp.asarray(tallies, jnp.int32))

    tallies = jnp.where(number % 4 == 0, named(packed, number // 4), named(ordinary, number - number // 4 - 1))
    mixed = jax.random.permutation(jax.random.fold_in(own, 3), count)
    donor, receiver = mixed[0:count // 2 * 2:2], mixed[1:count // 2 * 2:2]
    margin = jnp.minimum(tallies[donor] - 1, reach - tallies[receiver]) // 2
    margin = jnp.where((donor == ranking[0]) | (receiver == ranking[0]) | (tallies[receiver] == 0), 0, jnp.maximum(margin, 0))
    shifted = jax.random.randint(jax.random.fold_in(own, 4), (count // 2,), 0, 1 << 20) % (margin + 1)
    tallies = tallies.at[donor].add(-shifted).at[receiver].add(shifted)
    items = jnp.searchsorted(jnp.cumsum(tallies), jnp.arange(rows * top), side="right").astype(jnp.int32)
    table = items.reshape(top, rows).T
    table = table[jax.random.permutation(jax.random.fold_in(own, 1), rows)]
    offset_by = jax.random.randint(jax.random.fold_in(own, 2), (rows, 1), 0, top)
    return jnp.take_along_axis(table, (jnp.arange(top)[None, :] + offset_by) % top, axis=1)


def shares(number_of, total, bound, lean, full):
    portions = [(1 << 20) // math.isqrt(grade ** lean) + 1 for grade in range(1, number_of + 1)]
    largest = bound if full else min(bound, max(-(-total // number_of), total * portions[0] // sum(portions)))
    least = 1 if total - largest >= number_of - 1 else 0
    counts, surplus = [largest] + [least] * (number_of - 1), total - largest - least * (number_of - 1)
    while surplus > 0:
        candidates = [i for i in range(1, number_of) if counts[i] < largest] or [i for i in range(1, number_of) if counts[i] < bound]
        whole, left = sum([portions[i] for i in candidates]), surplus
        for i in candidates:
            more = min(bound - counts[i], max(1, left * portions[i] // whole), surplus)
            counts[i] = counts[i] + more
            surplus = surplus - more
    return np.array(counts)


def noise(stream_key, shape, scale, most, pieces=(), kind=jnp.bfloat16):
    values = jax.random.normal(stream_key, shape, jnp.float32) * scale
    if len(pieces) > 0:
        values = block_levels(stream_key, shape, pieces, -0.22, 0.18) * values
    return jnp.clip(values, min=-most, max=most).astype(kind)


def setup_inputs(seed: int = 0) -> dict:
    key_list = jax.random.split(jax.random.key(seed), 21)
    hidden_in = noise(key_list[0], (SEQS, D), 1.0, 6.0, ((0, 128),))
    lengths = draw_lengths(jax.random.fold_in(key_list[20], 71), 0)
    key_cache = draw_key_cache(jax.random.fold_in(key_list[20], 71), 0)
    value_cache = noise(key_list[3], (SEQS, CACHE, KV_HEADS * VALUE_DIM), 1.0, 6.0, ((0, 128),))
    query_w = noise(key_list[4], (D, HEADS * 2 * HEAD_DIM), D ** -0.5, 0.125, ((0, 128),))
    key_w = noise(key_list[5], (D, KV_HEADS * 2 * HEAD_DIM), D ** -0.5, 0.125, ((0, 128),))
    value_w = noise(key_list[6], (D, KV_HEADS * VALUE_DIM), D ** -0.5, 0.125, ((0, 128),))
    out_w = noise(key_list[7], (HEADS * VALUE_DIM, D), (HEADS * VALUE_DIM) ** -0.5, 0.125, ((0, 128),))
    lam_heads = jnp.clip(jax.random.uniform(key_list[8], (HEADS,), jnp.float32, 0.3, 0.8), 0.3, 0.8)
    head_gain = jnp.clip(1.0 + 0.18 * jax.random.normal(key_list[9], (VALUE_DIM,), jnp.float32), 0.1, 1.9)
    attn_gain = jnp.clip(1.0 + 0.18 * jax.random.normal(key_list[10], (D,), jnp.float32), 0.1, 1.9)
    moe_gain = jnp.clip(1.0 + 0.18 * jax.random.normal(key_list[11], (D,), jnp.float32), 0.1, 1.9)
    routing_keys = jax.random.split(jax.random.fold_in(key_list[12], 1), SEQS // SEQS)
    routing_turns = jax.random.permutation(jax.random.fold_in(key_list[12], 3), SEQS // SEQS)
    routing = jax.vmap(lambda own, number: deal_out(jax.random.fold_in(key_list[12], 2), own, number, SEQS, EXPERTS, TOPK, EXP_CAP, 1))(routing_keys, routing_turns).reshape((SEQS, TOPK))
    route_weight = jnp.clip(jnp.exp(jax.random.uniform(key_list[13], (SEQS, TOPK), jnp.float32, math.log(0.1), math.log(0.6))), 0.1, 0.6)
    gate_w = noise(key_list[14], (EXPERTS, D, EXPERT_DIM), D ** -0.5, 0.125, ((0, 128),))
    up_w = noise(key_list[15], (EXPERTS, D, EXPERT_DIM), D ** -0.5, 0.125, ((0, 128),))
    down_w = noise(key_list[16], (EXPERTS, EXPERT_DIM, D), EXPERT_DIM ** -0.5, 0.25, ((0, 128),))
    shared_gate = noise(key_list[17], (D, SHARED_DIM), D ** -0.5, 0.125)
    shared_up = noise(key_list[18], (D, SHARED_DIM), D ** -0.5, 0.125)
    shared_down = noise(key_list[19], (SHARED_DIM, D), SHARED_DIM ** -0.5, 0.25)
    return dict(hidden_in=hidden_in, lengths=lengths, key_cache=key_cache, value_cache=value_cache, query_w=query_w, key_w=key_w, value_w=value_w, out_w=out_w, lam_heads=lam_heads, head_gain=head_gain, attn_gain=attn_gain, moe_gain=moe_gain, routing=routing, route_weight=route_weight, gate_w=gate_w, up_w=up_w, down_w=down_w, shared_gate=shared_gate, shared_up=shared_up, shared_down=shared_down)


eps_norm = 1e-06
eps_head = 1e-05
theta_base = 500000.0

def rms_scale(row_block, gain_vec, epsilon):
    row_block = row_block.astype(jnp.float32)
    return row_block * lax.rsqrt(lax.optimization_barrier(jnp.mean(row_block * row_block, axis=-1, keepdims=True)) + epsilon) * gain_vec.astype(jnp.float32)

def rotate(vectors, positions):
    half_width = vectors.shape[-1] // 2
    inverse = theta_base ** (-jnp.arange(half_width, dtype=jnp.float32) / half_width)
    angles = positions.astype(jnp.float32)[..., None] * inverse
    cosine, sine_part = (jnp.cos(angles), jnp.sin(angles))
    lower_half, upper_half = (vectors[..., :half_width], vectors[..., half_width:])
    return jnp.concatenate([lower_half * cosine - upper_half * sine_part, lower_half * sine_part + upper_half * cosine], axis=-1)

def attend(queries, key_new, value_new, cache_keys, cache_values, lengths, lam_heads, head_gain):
    num_seqs, kv_heads, group_size = (queries.shape[0], queries.shape[1], queries.shape[2])
    head_dim = queries.shape[-1]
    cache_len = cache_keys.shape[1]
    cache_keys = cache_keys.reshape(num_seqs, cache_len, kv_heads, 2, head_dim).astype(jnp.float32)
    cache_values = cache_values.reshape(num_seqs, cache_len, kv_heads, -1).astype(jnp.float32)
    value_new = value_new.reshape(num_seqs, kv_heads, -1)
    queries = queries.astype(jnp.float32)
    score_scale = head_dim ** (-0.5)
    scores = jnp.einsum('skgph,sckph->skgpc', queries, cache_keys) * score_scale
    self_score = jnp.einsum('skgph,skph->skgp', queries, key_new.astype(jnp.float32)) * score_scale
    live_mask = (jnp.arange(cache_len)[None, :] < lengths[:, None])[:, None, None, None, :]
    peak = jnp.maximum(lax.optimization_barrier(jnp.max(jnp.where(live_mask, scores, -jnp.inf), axis=-1)), self_score)
    weights = jnp.where(live_mask, jnp.exp(scores - peak[..., None]), 0.0)
    self_weight = jnp.exp(self_score - peak)
    totals = lax.optimization_barrier(jnp.sum(weights, axis=-1)) + self_weight
    lambda_grid = lam_heads.reshape(kv_heads, group_size)[None]
    combined = (weights[:, :, :, 0] / totals[:, :, :, 0, None] - lambda_grid[..., None] * weights[:, :, :, 1] / totals[:, :, :, 1, None]).astype(jnp.bfloat16)
    self_combined = (self_weight[..., 0] / totals[..., 0] - lambda_grid * self_weight[..., 1] / totals[..., 1]).astype(jnp.bfloat16)
    head_out = jnp.einsum('skgc,sckv->skgv', combined.astype(jnp.float32), cache_values)
    head_out = head_out + self_combined.astype(jnp.float32)[..., None] * value_new.astype(jnp.float32)[:, :, None, :]
    return rms_scale(head_out, head_gain, eps_head).astype(jnp.bfloat16).reshape(num_seqs, -1)

def routed_sum(moe_in, routing, route_weight, gate_w, up_w, down_w):

    def add_expert(running, expert_id):
        routed_here = lax.optimization_barrier(jnp.sum((routing == expert_id).astype(jnp.int32), axis=1))
        weight_col = lax.optimization_barrier(jnp.sum(jnp.where(routing == expert_id, route_weight, 0.0), axis=1))
        slot_index = jnp.cumsum(routed_here) - 1
        pick_table = ((slot_index[None, :] == jnp.arange(EXP_CAP)[:, None]) & (routed_here[None, :] > 0)).astype(jnp.float32)
        picked = jnp.dot(pick_table, moe_in.astype(jnp.float32)).astype(jnp.bfloat16)
        gate_one = lax.dynamic_index_in_dim(gate_w, expert_id, 0, keepdims=False)
        up_one = lax.dynamic_index_in_dim(up_w, expert_id, 0, keepdims=False)
        down_one = lax.dynamic_index_in_dim(down_w, expert_id, 0, keepdims=False)
        hidden = (jax.nn.silu(jnp.dot(picked, gate_one, preferred_element_type=jnp.float32)) * jnp.dot(picked, up_one, preferred_element_type=jnp.float32)).astype(jnp.bfloat16)
        result = jnp.dot(hidden, down_one, preferred_element_type=jnp.float32).astype(jnp.bfloat16)
        return (running + jnp.dot(pick_table.T, result.astype(jnp.float32)) * weight_col[:, None], None)
    start_sum = jnp.zeros(moe_in.shape, jnp.float32)
    running, unused = lax.scan(add_expert, start_sum, jnp.arange(gate_w.shape[0], dtype=jnp.int32))
    return running

def reference(hidden_in, lengths, key_cache, value_cache, query_w, key_w, value_w, out_w, lam_heads, head_gain, attn_gain, moe_gain, routing, route_weight, gate_w, up_w, down_w, shared_gate, shared_up, shared_down):
    num_seqs = hidden_in.shape[0]
    normed = rms_scale(hidden_in, attn_gain, eps_norm).astype(jnp.bfloat16)
    q_raw = jnp.dot(normed, query_w, preferred_element_type=jnp.float32)
    k_raw = jnp.dot(normed, key_w, preferred_element_type=jnp.float32)
    value_new = jnp.dot(normed, value_w, preferred_element_type=jnp.float32).astype(jnp.bfloat16)
    queries = rotate(q_raw.reshape(num_seqs, KV_HEADS, -1, 2, HEAD_DIM), lengths[:, None, None, None]).astype(jnp.bfloat16)
    key_new = rotate(k_raw.reshape(num_seqs, KV_HEADS, 2, HEAD_DIM), lengths[:, None, None]).astype(jnp.bfloat16)

    def one_sequence(items):
        return attend(*[item[None] for item in items], lam_heads, head_gain)[0]
    attn_out = lax.map(one_sequence, (queries, key_new, value_new, key_cache, value_cache, lengths))
    attn_proj = jnp.dot(attn_out, out_w, preferred_element_type=jnp.float32).astype(jnp.bfloat16)
    after_mixer = (hidden_in.astype(jnp.float32) + attn_proj.astype(jnp.float32)).astype(jnp.bfloat16)
    moe_in = rms_scale(after_mixer, moe_gain, eps_norm).astype(jnp.bfloat16)
    routed = routed_sum(moe_in, routing, route_weight, gate_w, up_w, down_w)
    shared_hidden = (jax.nn.silu(jnp.dot(moe_in, shared_gate, preferred_element_type=jnp.float32)) * jnp.dot(moe_in, shared_up, preferred_element_type=jnp.float32)).astype(jnp.bfloat16)
    shared_out = jnp.dot(shared_hidden, shared_down, preferred_element_type=jnp.float32)
    layer_out = (after_mixer.astype(jnp.float32) + routed + shared_out).astype(jnp.bfloat16)
    return (layer_out, key_new.reshape(num_seqs, -1), value_new)
```

```python
import jax
import jax.numpy as jnp
from jax import lax
from jax.sharding import Mesh
from jax.sharding import PartitionSpec as P

KV_HEADS = 2
HEAD_DIM = 128
EXP_CAP = 24
SLOTS = 32
AXES = ("z", "yh", "yl", "x", "c")
INNER = ("yl", "x", "c")
CHIPS = ("z", "yh", "yl", "x")

eps_norm = 1e-06
eps_head = 1e-05
theta_base = 500000.0
f32 = jnp.float32
bf16 = jnp.bfloat16


def exchange(value, axes):
    return lax.all_to_all(value, axes, split_axis=0, concat_axis=0, tiled=True)


def pair_swap(value):
    return lax.ppermute(value, "c", [(0, 1), (1, 0)])


def rms_scale(rows, gain, epsilon):
    rows = rows.astype(f32)
    return rows * lax.rsqrt(jnp.mean(rows * rows, axis=-1, keepdims=True) + epsilon) * gain


def rotate(vectors, positions):
    half_width = vectors.shape[-1] // 2
    inverse = theta_base ** (-jnp.arange(half_width, dtype=f32) / half_width)
    angles = positions.astype(f32)[..., None] * inverse
    cosine, sine = jnp.cos(angles), jnp.sin(angles)
    lower, upper = vectors[..., :half_width], vectors[..., half_width:]
    return jnp.concatenate([lower * cosine - upper * sine, lower * sine + upper * cosine], axis=-1)


def attend(queries, key_new, value_new, cache_keys, cache_values, lengths, lam_heads, head_gain):
    num_seqs, kv_heads, group_size = queries.shape[:3]
    head_dim = queries.shape[-1]
    cache_len = cache_keys.shape[1]
    cache_keys = cache_keys.reshape(num_seqs, cache_len, kv_heads, 2, head_dim)
    cache_values = cache_values.reshape(num_seqs, cache_len, kv_heads, -1)
    value_new = value_new.reshape(num_seqs, kv_heads, -1)
    score_scale = head_dim ** (-0.5)
    scores = (
        jnp.einsum("skgph,sckph->skgpc", queries, cache_keys, preferred_element_type=f32)
        * score_scale
    )
    self_score = (
        jnp.einsum("skgph,skph->skgp", queries, key_new, preferred_element_type=f32) * score_scale
    )
    live = (jnp.arange(cache_len)[None, :] < lengths[:, None])[:, None, None, None, :]
    peak = jnp.maximum(jnp.max(jnp.where(live, scores, -jnp.inf), axis=-1), self_score)
    weights = jnp.where(live, jnp.exp(scores - peak[..., None]), 0.0)
    self_weight = jnp.exp(self_score - peak)
    totals = jnp.sum(weights, axis=-1) + self_weight
    lam = lam_heads.reshape(kv_heads, group_size)[None]
    combined = (
        weights[:, :, :, 0] / totals[:, :, :, 0, None]
        - lam[..., None] * weights[:, :, :, 1] / totals[:, :, :, 1, None]
    ).astype(bf16)
    self_combined = (
        self_weight[..., 0] / totals[..., 0] - lam * self_weight[..., 1] / totals[..., 1]
    ).astype(bf16)
    head_out = jnp.einsum("skgc,sckv->skgv", combined, cache_values, preferred_element_type=f32)
    head_out = (
        head_out + self_combined.astype(f32)[..., None] * value_new.astype(f32)[:, :, None, :]
    )
    return rms_scale(head_out, head_gain, eps_head).astype(bf16).reshape(num_seqs, -1)


def on_device(
    hidden_in,
    lengths,
    key_cache,
    value_cache,
    query_w,
    key_w,
    value_w,
    out_w,
    lam_heads,
    head_gain,
    attn_gain,
    moe_gain,
    routing,
    route_weight,
    gate_w,
    up_w,
    down_w,
    shared_gate,
    shared_up,
    shared_down,
):
    n = lax.axis_size(AXES)
    device = lax.axis_index(AXES)
    core = lax.axis_index("c")
    chips = n // 2
    tok, width = hidden_in.shape
    tokens = tok * n
    inner = lax.axis_size(INNER)
    outer = n // inner
    span = width // outer
    cols = width // n

    normed = rms_scale(hidden_in, attn_gain, eps_norm).astype(bf16)
    slices = jnp.moveaxis(normed.reshape(tok, outer, span), 1, 0)
    slices = jnp.broadcast_to(slices[:, None], (outer, inner, tok, span)).reshape(n, tok, span)
    hidden_cols = hidden_in.reshape(tok, cols, n).transpose(2, 0, 1)
    arrived = exchange(jnp.concatenate([slices, hidden_cols], axis=2), AXES)
    rows = query_w.shape[0]
    blocks = [
        w.reshape(rows, inner, w.shape[1] // inner).transpose(1, 0, 2)
        for w in (query_w, key_w, value_w)
    ]
    qkv_w = exchange(jnp.concatenate(blocks, axis=2), INNER).reshape(span, -1)
    token_part = arrived[:, :, :span].reshape(tokens, span)
    hidden_part = arrived[:, :, span:].reshape(tokens, cols)

    ow = out_w.reshape(rows * cols, n).T.reshape(chips, 1, 2 * rows * cols)
    ow = jnp.broadcast_to(ow, (chips, 2, 2 * rows * cols)).reshape(n, -1, 128)
    ow = exchange(ow, AXES)
    ow = lax.dynamic_slice_in_dim(ow, core * chips, chips, 0)
    ow = ow.reshape(chips, 2, rows, cols).transpose(0, 2, 1, 3).reshape(chips * rows, 2 * cols)

    sums = jnp.dot(token_part, qkv_w, preferred_element_type=f32)
    sums = exchange(sums.reshape(n, tok, -1), AXES)
    sums = sums.reshape(outer, inner, tok, -1).sum(axis=0)
    q_part = query_w.shape[1] // inner
    k_part = key_w.shape[1] // inner
    q_raw = sums[:, :, :q_part].transpose(1, 0, 2)
    k_raw = sums[:, :, q_part : q_part + k_part].transpose(1, 0, 2)
    value_new = sums[:, :, q_part + k_part :].transpose(1, 0, 2).reshape(tok, -1).astype(bf16)
    queries = rotate(
        q_raw.reshape(tok, KV_HEADS, -1, 2, HEAD_DIM), lengths[:, None, None, None]
    ).astype(bf16)
    key_new = rotate(
        k_raw.reshape(tok, KV_HEADS, 2, HEAD_DIM), lengths[:, None, None]
    ).astype(bf16)
    attn_out = attend(
        queries, key_new, value_new, key_cache, value_cache, lengths, lam_heads, head_gain
    )

    half = width // 2
    pieces = jnp.moveaxis(attn_out.reshape(tok, 2, half), 1, 0)
    pieces = jnp.broadcast_to(pieces[None], (chips, 2, tok, half)).reshape(n, tok, half)
    pieces = exchange(pieces, AXES).reshape(tokens, half)
    partial = jnp.dot(pieces, ow, preferred_element_type=f32)
    mine = jnp.where(core == 0, partial[:, :cols], partial[:, cols:])
    theirs = jnp.where(core == 0, partial[:, cols:], partial[:, :cols])
    attn_proj = (mine + pair_swap(theirs)).astype(bf16)
    mixed_cols = (hidden_part.astype(f32) + attn_proj.astype(f32)).astype(bf16)

    ids = jnp.arange(n, dtype=jnp.int32)
    match = routing[:, :, None] == ids
    named = jnp.any(match, axis=1)
    weight_of = jnp.sum(jnp.where(match, route_weight[:, :, None], 0.0), axis=1)
    t_ids = jnp.arange(tokens, dtype=jnp.int32)
    below = (t_ids[:, None] >= t_ids[None, :]).astype(bf16)
    slot = jnp.dot(below, named.astype(bf16), preferred_element_type=f32).astype(jnp.int32) - 1
    slot = jnp.where(named, slot, -1)
    s_ids = jnp.arange(SLOTS, dtype=jnp.int32)
    pick = slot.T[:, None, :] == s_ids[None, :, None]
    own = t_ids[None, None, :] == (ids[:, None] * tok + s_ids[None, :] - EXP_CAP)[:, :, None]
    last = (s_ids >= EXP_CAP) & (s_ids < EXP_CAP + tok)
    pick = jnp.where(last[None, :, None], own, pick & (s_ids < EXP_CAP)[None, :, None])
    pick = pick.astype(bf16)

    chosen = jnp.dot(pick.reshape(n * SLOTS, tokens), mixed_cols, preferred_element_type=f32)
    chosen = chosen.astype(bf16).reshape(n, SLOTS * cols // 128, 128)
    chosen = exchange(chosen, AXES).reshape(n, SLOTS, cols)
    mixed = chosen.transpose(1, 2, 0).reshape(SLOTS, width)
    moe_in = rms_scale(mixed, moe_gain, eps_norm).astype(bf16)
    hidden = (
        jax.nn.silu(jnp.dot(moe_in, gate_w[0], preferred_element_type=f32))
        * jnp.dot(moe_in, up_w[0], preferred_element_type=f32)
    ).astype(bf16)
    result = jnp.dot(hidden, down_w[0], preferred_element_type=f32).astype(bf16)

    kept = lax.dynamic_slice_in_dim(result, core * half, half, 1)
    given = lax.dynamic_slice_in_dim(result, (1 - core) * half, half, 1)
    given = pair_swap(given[:EXP_CAP])
    stacked = jnp.concatenate([kept[:EXP_CAP], given], axis=0)

    def spread(expert):
        sl = lax.dynamic_slice_in_dim(slot, expert, 1, 1)
        w = lax.dynamic_slice_in_dim(weight_of, expert, 1, 1)
        return jnp.where(sl == s_ids[None, :EXP_CAP], w, 0.0)

    table = jnp.concatenate([spread(device), spread(device + 1 - 2 * core)], axis=1)
    high = table.astype(bf16)
    low = (table - high.astype(f32)).astype(bf16)
    summed = jnp.dot(
        jnp.concatenate([high, low], axis=1),
        jnp.concatenate([stacked, stacked], axis=0),
        preferred_element_type=f32,
    ).astype(bf16)
    back = exchange(summed.reshape(n, tok, half), AXES)
    routed = jnp.sum(back.reshape(chips, 2, tok, half).astype(f32), axis=0)
    routed = jnp.moveaxis(routed, 0, 1).reshape(tok, width)

    after_mixer = mixed[EXP_CAP : EXP_CAP + tok]
    own_in = moe_in[EXP_CAP : EXP_CAP + tok]
    shared_hidden = (
        jax.nn.silu(jnp.dot(own_in, shared_gate, preferred_element_type=f32))
        * jnp.dot(own_in, shared_up, preferred_element_type=f32)
    ).astype(bf16)
    shared_out = jnp.dot(shared_hidden, shared_down, preferred_element_type=f32)
    layer_out = (after_mixer.astype(f32) + routed + shared_out).astype(bf16)
    return (layer_out, key_new.reshape(tok, -1), value_new)


def solution(mesh):
    torus = Mesh(mesh.devices.reshape(4, 2, 2, 4, 2), AXES)
    split = P(AXES)
    return jax.shard_map(
        on_device,
        mesh=torus,
        in_specs=(split,) * 8 + (P(),) * 6 + (split,) * 3 + (P(),) * 3,
        out_specs=(split, split, split),
        check_vma=False,
    )
```
